32 devices in a mesh: sp: 16 (over z, y, x), tp: 2 (over core).
Axes of the slice: x: 2, y: 2, z: 4, core: 2. Of those that a mesh axis runs over, the one named last changes fastest.
Arguments:
- tokens: bfloat16 [4096, 2048], P('sp', 'tp'), may hold values from -6 to 6
- norm_gain: float32 [2, 2048], replicated, may hold values from 0.1 to 1.9
- w_bgate: bfloat16 [2, 2048, 2048], P(None, 'sp', 'tp'), may hold values from -0.125 to 0.125
- w_cgate: bfloat16 [2, 2048, 2048], P(None, 'sp', 'tp'), may hold values from -0.125 to 0.125
- w_value: bfloat16 [2, 2048, 2048], P(None, 'sp', 'tp'), may hold values from -0.125 to 0.125
- conv_taps: float32 [2, 3, 2048], replicated, may hold values from -3.5 to 3.5
- w_out: bfloat16 [2, 2048, 2048], P(None, 'sp', 'tp'), may hold values from -0.125 to 0.125
Outputs:
- mixed_out: bfloat16 [4096, 2048], P('sp', 'tp')
The draws below stay inside these ranges and needn't reach their ends.
All inputs are finite; a program needn't handle non-finite values.
Results may differ from the reference program's by a relative error of at most 0.015.
Values may be sent and summed in bfloat16 or wider, within the bound.
A program may use at most 64 MiB of HBM per device.

```python
import jax
import jax.numpy as jnp
from jax import lax

D = 2048
LAYERS = 2
SEQ = 4096


def steps_of(stream_key, dims, pieces, low, largest):
    gain, own = 1.0, jax.random.fold_in(stream_key, 6)
    for axis_at, blocks in pieces:
        heights = jnp.exp(jax.random.uniform(jax.random.fold_in(own, axis_at), (blocks,), jnp.float32, low / len(pieces), largest / len(pieces)))
        gain = gain * jnp.repeat(heights, dims[axis_at] // blocks).reshape([-1 if axis == axis_at else 1 for axis in range(len(dims))])
    return gain


def bell_draw(stream_key, dims, width, limit, shards=(), kind=jnp.bfloat16):
    loudness = steps_of(stream_key, dims, shards, -0.22, 0.18) if shards else 1.0
    entries = jax.random.normal(stream_key, dims, jnp.float32) * width * loudness
    return jnp.minimum(jnp.maximum(entries, -limit), limit).astype(kind)


def setup_inputs(seed: int = 0) -> dict:
    key_of = jax.random.split(jax.random.key(seed), 8)
    tokens = bell_draw(key_of[0], (SEQ, D), 1.0, 6.0, ((0, 16), (1, 2)))
    norm_gain = jnp.clip(1.0 + 0.18 * jax.random.normal(key_of[1], (LAYERS, D), jnp.float32), 0.1, 1.9)
    w_bgate = bell_draw(key_of[2], (LAYERS, D, D), D ** -0.5, 0.125, ((1, 16), (2, 2)))
    w_cgate = bell_draw(key_of[3], (LAYERS, D, D), D ** -0.5, 0.125, ((1, 16), (2, 2)))
    w_value = bell_draw(key_of[4], (LAYERS, D, D), D ** -0.5, 0.125, ((1, 16), (2, 2)))
    conv_taps = bell_draw(key_of[5], (LAYERS, 3, D), 3 ** -0.5, 3.5, (), jnp.float32)
    w_out = bell_draw(key_of[6], (LAYERS, D, D), D ** -0.5, 0.125, ((1, 16), (2, 2)))
    return {"tokens": tokens, "norm_gain": norm_gain, "w_bgate": w_bgate, "w_cgate": w_cgate, "w_value": w_value, "conv_taps": conv_taps, "w_out": w_out}


def reference(tokens, norm_gain, w_bgate, w_cgate, w_value, conv_taps, w_out):
    current = tokens
    for layer_idx in range(LAYERS):
        as_float = current.astype(jnp.float32)
        scale = lax.rsqrt(lax.optimization_barrier(jnp.mean(as_float * as_float, axis=-1, keepdims=True)) + 1e-06)
        normed = (as_float * scale * norm_gain[layer_idx].astype(jnp.float32)).astype(jnp.bfloat16)
        bgate = lax.optimization_barrier(jnp.dot(normed, w_bgate[layer_idx], preferred_element_type=jnp.float32).astype(jnp.bfloat16))
        cgate = lax.optimization_barrier(jnp.dot(normed, w_cgate[layer_idx], preferred_element_type=jnp.float32).astype(jnp.bfloat16))
        values = lax.optimization_barrier(jnp.dot(normed, w_value[layer_idx], preferred_element_type=jnp.float32).astype(jnp.bfloat16))
        product = cgate.astype(jnp.float32) * values.astype(jnp.float32)
        padded = jnp.pad(product, ((2, 0), (0, 0)))
        taps = conv_taps[layer_idx]
        mixed = taps[0] * padded[:-2] + taps[1] * padded[1:-1] + taps[2] * padded[2:]
        gated = (bgate.astype(jnp.float32) * mixed).astype(jnp.bfloat16)
        update = jnp.dot(gated, w_out[layer_idx], preferred_element_type=jnp.float32)
        current = (as_float + update).astype(jnp.bfloat16)
    return current
```

```python
import functools

import jax
import jax.numpy as jnp
from jax import lax
from jax.experimental import pallas as pl
from jax.experimental.pallas import tpu as pltpu
from jax.sharding import PartitionSpec as P

MESH = pl.DeviceIdType.MESH
LANES = 128
AHEAD = 2
F32 = jnp.float32
BF16 = jnp.bfloat16


def mixer_kernel(dims, tok, gain, wb, wc, wv, taps, wo, out,
                 acts, gates, normed, weights, product, cgate, result, landed,
                 loc_sem, plane_send, plane_recv, line_send, line_recv,
                 ag_send, ag_recv, pair_send, pair_recv,
                 halo_send, halo_recv, out_send, out_recv):
    depth, group, line, tps, rows, cols, width, krows = dims
    span = rows * group
    block = krows * group
    chunks = [(l, m) for l in range(depth) for m in range(4)]
    sources = (wc, wv, wb, wo)
    sp, t = lax.axis_index("sp"), lax.axis_index("tp")
    z, q = sp // group, sp % group
    own = pl.multiple_of(t * cols + q * width, width)
    tile = min(256, span)

    def in_plane(d):
        return (z * group + (q + d) % group, t)

    def in_pair(d):
        return (sp, (t + d) % tps)

    def remote(src, dst, send, recv, device):
        return pltpu.make_async_remote_copy(src_ref=src, dst_ref=dst, send_sem=send, recv_sem=recv,
                                            device_id=device, device_id_type=MESH)

    barrier = pltpu.get_barrier_semaphore()

    def hello(device):
        pl.semaphore_signal(barrier, inc=1, device_id=device, device_id_type=MESH)

    for d in range(1, group):
        hello(in_plane(d))
    for d in range(1, tps):
        hello(in_pair(d))

    @pl.when(z > 0)
    def _():
        hello((sp - group, t))

    @pl.when(z < line - 1)
    def _():
        hello((sp + group, t))

    pl.semaphore_wait(barrier, group - 1 + tps - 1
                      + jnp.where(z > 0, 1, 0) + jnp.where(z < line - 1, 1, 0))

    def weight_rows(i, zz, qq):
        l, m = chunks[i]
        return weights.at[l, m, pl.ds(pl.multiple_of((zz * group + qq) * krows, krows), krows), :]

    def weight_block(i, zz):
        l, m = chunks[i]
        return weights.at[l, m, pl.ds(pl.multiple_of(zz * block, block), block), :]

    def weight_source(i, qq):
        l, m = chunks[i]
        return sources[m].at[l, :, pl.ds(pl.multiple_of(qq * width, width), width)]

    def plane_copy(i, d, sender):
        return remote(weight_source(i, (q + d) % group), weight_rows(i, z, sender),
                      plane_send.at[i, d], plane_recv.at[i, d], in_plane(d))

    def local_copy(i):
        return pltpu.make_async_copy(weight_source(i, q), weight_rows(i, z, q), loc_sem.at[i])

    def line_copy(i, zz, up):
        blk = weight_block(i, zz)
        return remote(blk, blk, line_send.at[0 if up else 1, i, zz], line_recv.at[i, zz],
                      (sp + group, t) if up else (sp - group, t))

    def plane_start(i):
        local_copy(i).start()
        for d in range(1, group):
            plane_copy(i, d, q).start()

    def line_start(i):
        local_copy(i).wait()
        for d in range(1, group):
            plane_copy(i, d, (q + group - d) % group).wait_recv()

        @pl.when(z < line - 1)
        def _():
            line_copy(i, z, True).start()

        @pl.when(z > 0)
        def _():
            line_copy(i, z, False).start()

    def line_round(i):
        if i + AHEAD < len(chunks):
            line_start(i + AHEAD)

        def step(j, carry):
            below, above = z - 1 - j, z + 1 + j

            @pl.when(below >= 0)
            def _():
                line_copy(i, below, True).wait_recv()

                @pl.when(z < line - 1)
                def _():
                    line_copy(i, below, True).start()

            @pl.when(above < line)
            def _():
                line_copy(i, above, False).wait_recv()

                @pl.when(z > 0)
                def _():
                    line_copy(i, above, False).start()

            return carry

        lax.fori_loop(0, line - 1, step, 0)

    def act_slice(ph, tt, qq):
        l = ph // 2
        if ph == 0:
            return acts.at[0, pl.ds(pl.multiple_of(qq * rows, rows), rows),
                           pl.ds(pl.multiple_of(tt * cols, cols), cols)]
        buf = acts if ph % 2 == 0 else gates
        return buf.at[l, :, pl.ds(pl.multiple_of(tt * cols + qq * width, width), width)]

    def ag_copy(ph, d, qq):
        src = tok if ph == 0 else act_slice(ph, t, q)
        return remote(src, act_slice(ph, t, qq), ag_send.at[ph, d], ag_recv.at[ph, d], in_plane(d))

    def pair_copy(ph, dq, d, tt):
        qq = (q + group - dq) % group
        src = tok if ph == 0 and dq == 0 else act_slice(ph, t, qq)
        return remote(src, act_slice(ph, tt, qq), pair_send.at[ph, dq, d], pair_recv.at[ph, dq, d],
                      in_pair(d))

    def gather_start(ph):
        for d in range(1, group):
            ag_copy(ph, d, q).start()
        for d in range(1, tps):
            pair_copy(ph, 0, d, t).start()

    def gather_finish(ph):
        for d in range(1, group):
            ag_copy(ph, d, (q + group - d) % group).wait_recv()
            for e in range(1, tps):
                pair_copy(ph, d, e, t).start()
        for d in range(group):
            for e in range(1, tps):
                pair_copy(ph, d, e, (t + tps - e) % tps).wait_recv()

    def tiles(body):
        def step(i, carry):
            body(pl.multiple_of(i * tile, tile))
            return carry

        lax.fori_loop(0, span // tile, step, 0)

    def normalize(l):
        sub = 32

        def step(i, carry):
            at = pl.ds(pl.multiple_of(i * sub, sub), sub)
            x = acts[l, at, :].astype(F32)
            scale = lax.rsqrt(jnp.mean(x * x, axis=-1, keepdims=True) + 1e-06)
            normed[at, :] = (x * scale * gain[pl.ds(l, 1), :]).astype(BF16)
            return carry

        lax.fori_loop(0, span // sub, step, 0)

    def project(l, m, r):
        return jnp.dot(normed[pl.ds(r, tile), :], weights[l, m], preferred_element_type=F32).astype(BF16)

    def halo_copy(l):
        return remote(product.at[l, pl.ds(span, 8), :], product.at[l, pl.ds(0, 8), :],
                      halo_send.at[l], halo_recv.at[l], (sp + group, t))

    def do_cgate(l):
        def body(r):
            cgate[pl.ds(r, tile), :] = project(l, 0, r)
        tiles(body)

    def do_values(l):
        def body(r):
            values = project(l, 1, r)
            product[l, pl.ds(r + 8, tile), :] = cgate[pl.ds(r, tile), :].astype(F32) * values.astype(F32)
        tiles(body)

        @pl.when(z < line - 1)
        def _():
            halo_copy(l).start()

    def do_bgate(l):
        @pl.when(z > 0)
        def _():
            halo_copy(l).wait_recv()

        @pl.when(z == 0)
        def _():
            product[l, pl.ds(0, 8), :] = jnp.zeros((8, width), F32)

        tap = [taps[l, pl.ds(k, 1), pl.ds(own, width)] for k in range(3)]

        def body(r):
            bgate = project(l, 2, r).astype(F32)
            near = product[l, pl.ds(r, tile + 8), :]
            mixed = tap[0] * near[6:6 + tile] + tap[1] * near[7:7 + tile] + tap[2] * near[8:8 + tile]
            gates[l, pl.ds(r, tile), pl.ds(own, width)] = (bgate * mixed).astype(BF16)
        tiles(body)

    def do_out(l):
        def body(r):
            update = jnp.dot(gates[l, pl.ds(r, tile), :], weights[l, 3], preferred_element_type=F32)
            current = (acts[l, pl.ds(r, tile), pl.ds(own, width)].astype(F32) + update).astype(BF16)
            if l + 1 < depth:
                acts[l + 1, pl.ds(r, tile), pl.ds(own, width)] = current
            else:
                result[pl.ds(r, tile), :] = current
        tiles(body)

    def out_copy(d, qq):
        return remote(result.at[pl.ds(pl.multiple_of((q + d) % group * rows, rows), rows), :],
                      landed.at[:, pl.ds(pl.multiple_of(qq * width, width), width)],
                      out_send.at[d], out_recv.at[d], in_plane(d))

    own_tokens = pltpu.make_async_copy(tok, act_slice(0, t, q), loc_sem.at[len(chunks)])
    plane_start(0)
    own_tokens.start()
    gather_start(0)
    for i in range(1, len(chunks)):
        plane_start(i)
    for i in range(min(AHEAD, len(chunks))):
        line_start(i)
    for l in range(depth):
        line_round(4 * l)
        if l == 0:
            own_tokens.wait()
        gather_finish(2 * l)
        normalize(l)
        do_cgate(l)
        line_round(4 * l + 1)
        do_values(l)
        line_round(4 * l + 2)
        do_bgate(l)
        gather_start(2 * l + 1)
        line_round(4 * l + 3)
        gather_finish(2 * l + 1)
        do_out(l)
        if l + 1 < depth:
            gather_start(2 * l + 2)
    for d in range(1, group):
        out_copy(d, q).start()
    landed[:, pl.ds(pl.multiple_of(q * width, width), width)] = result[
        pl.ds(pl.multiple_of(q * rows, rows), rows), :]
    for d in range(1, group):
        out_copy(d, (q + group - d) % group).wait_recv()
    out[...] = landed[...]

    for i in range(len(chunks)):
        for d in range(1, group):
            plane_copy(i, d, q).wait_send()

        def step(zz, carry):
            @pl.when((z < line - 1) & (zz <= z))
            def _():
                line_copy(i, zz, True).wait_send()

            @pl.when((z > 0) & (zz >= z))
            def _():
                line_copy(i, zz, False).wait_send()

            return carry

        lax.fori_loop(0, line, step, 0)
    for ph in range(2 * depth):
        for d in range(1, group):
            ag_copy(ph, d, q).wait_send()
        for d in range(group):
            for e in range(1, tps):
                pair_copy(ph, d, e, t).wait_send()
    for l in range(depth):
        @pl.when(z < line - 1)
        def _():
            halo_copy(l).wait_send()
    for d in range(1, group):
        out_copy(d, q).wait_send()


def shards(sp_size, tps, tokens, norm_gain, w_bgate, w_cgate, w_value, conv_taps, w_out):
    rows, cols = tokens.shape
    depth, krows, _ = w_bgate.shape
    group = 4
    while group > 1 and (sp_size % group or cols % (group * LANES)):
        group //= 2
    line = sp_size // group
    width = cols // group
    span = rows * group
    full = krows * sp_size
    n = 4 * depth
    dims = (depth, group, line, tps, rows, cols, width, krows)
    anywhere = pl.BlockSpec(memory_space=pl.ANY)
    vmem = pl.BlockSpec(memory_space=pltpu.VMEM)
    dma = pltpu.SemaphoreType.DMA
    return pl.pallas_call(
        functools.partial(mixer_kernel, dims),
        out_shape=jax.ShapeDtypeStruct((rows, cols), BF16),
        in_specs=[anywhere, vmem, anywhere, anywhere, anywhere, vmem, anywhere],
        out_specs=vmem,
        scratch_shapes=[
            pltpu.VMEM((depth, span, full), BF16),
            pltpu.VMEM((depth, span, full), BF16),
            pltpu.VMEM((span, full), BF16),
            pltpu.VMEM((depth, 4, full, width), BF16),
            pltpu.VMEM((depth, span + 8, width), F32),
            pltpu.VMEM((span, width), BF16),
            pltpu.VMEM((span, width), BF16),
            pltpu.VMEM((rows, cols), BF16),
            dma((n + 1,)), dma((n, group)), dma((n, group)),
            dma((2, n, line)), dma((n, line)),
            dma((2 * depth, group)), dma((2 * depth, group)),
            dma((2 * depth, group, tps)), dma((2 * depth, group, tps)),
            dma((depth,)), dma((depth,)), dma((group,)), dma((group,)),
        ],
        compiler_params=pltpu.CompilerParams(
            collective_id=0, has_side_effects=True, vmem_limit_bytes=60 * 1024 * 1024),
    )(tokens, norm_gain, w_bgate, w_cgate, w_value, conv_taps, w_out)


def solution(mesh):
    return jax.shard_map(
        functools.partial(shards, mesh.shape["sp"], mesh.shape["tp"]),
        mesh=mesh,
        in_specs=(
            P("sp", "tp"),
            P(),
            P(None, "sp", "tp"),
            P(None, "sp", "tp"),
            P(None, "sp", "tp"),
            P(),
            P(None, "sp", "tp"),
        ),
        out_specs=P("sp", "tp"),
        check_vma=False,
    )
```

```python
import functools

import jax
import jax.numpy as jnp
from jax import lax
from jax.experimental import pallas as pl
from jax.experimental.pallas import tpu as pltpu
from jax.sharding import PartitionSpec as P

MESH = pl.DeviceIdType.MESH
LANES = 128
AHEAD = 2
BEFORE_TOKENS = 2
F32 = jnp.float32
BF16 = jnp.bfloat16


def mixer_kernel(dims, tok, gain, wb, wc, wv, taps, wo, out,
                 acts, gates, normed, weights, product, cgate, result, landed,
                 loc_sem, plane_send, plane_recv, line_send, line_recv,
                 ag_send, ag_recv, pair_send, pair_recv,
                 halo_send, halo_recv, out_send, out_recv):
    depth, group, line, tps, rows, cols, width, krows = dims
    span = rows * group
    block = krows * group
    chunks = [(l, m) for l in range(depth) for m in range(4)]
    sources = (wc, wv, wb, wo)
    sp, t = lax.axis_index("sp"), lax.axis_index("tp")
    z, q = sp // group, sp % group
    own = pl.multiple_of(t * cols + q * width, width)
    tile = min(256, rows)

    def in_plane(d):
        return (z * group + (q + d) % group, t)

    def in_pair(d):
        return (sp, (t + d) % tps)

    def remote(src, dst, send, recv, device):
        return pltpu.make_async_remote_copy(src_ref=src, dst_ref=dst, send_sem=send, recv_sem=recv,
                                            device_id=device, device_id_type=MESH)

    barrier = pltpu.get_barrier_semaphore()

    def hello(device):
        pl.semaphore_signal(barrier, inc=1, device_id=device, device_id_type=MESH)

    for d in range(1, group):
        hello(in_plane(d))
    for d in range(1, tps):
        hello(in_pair(d))

    @pl.when(z > 0)
    def _():
        hello((sp - group, t))

    @pl.when(z < line - 1)
    def _():
        hello((sp + group, t))

    pl.semaphore_wait(barrier, group - 1 + tps - 1
                      + jnp.where(z > 0, 1, 0) + jnp.where(z < line - 1, 1, 0))

    def weight_rows(i, zz, qq):
        l, m = chunks[i]
        return weights.at[l, m, pl.ds(pl.multiple_of((zz * group + qq) * krows, krows), krows), :]

    def weight_block(i, zz):
        l, m = chunks[i]
        return weights.at[l, m, pl.ds(pl.multiple_of(zz * block, block), block), :]

    def weight_source(i, qq):
        l, m = chunks[i]
        return sources[m].at[l, :, pl.ds(pl.multiple_of(qq * width, width), width)]

    def plane_copy(i, d, sender):
        return remote(weight_source(i, (q + d) % group), weight_rows(i, z, sender),
                      plane_send.at[i, d], plane_recv.at[i, d], in_plane(d))

    def local_copy(i):
        return pltpu.make_async_copy(weight_source(i, q), weight_rows(i, z, q), loc_sem.at[i])

    def line_copy(i, zz, up):
        blk = weight_block(i, zz)
        return remote(blk, blk, line_send.at[0 if up else 1, i, zz], line_recv.at[i, zz],
                      (sp + group, t) if up else (sp - group, t))

    def plane_start(i):
        local_copy(i).start()
        for d in range(1, group):
            plane_copy(i, d, q).start()

    def line_start(i):
        local_copy(i).wait()
        for d in range(1, group):
            plane_copy(i, d, (q + group - d) % group).wait_recv()

        @pl.when(z < line - 1)
        def _():
            line_copy(i, z, True).start()

        @pl.when(z > 0)
        def _():
            line_copy(i, z, False).start()

    def line_round(i):
        def step(j, carry):
            below, above = z - 1 - j, z + 1 + j

            @pl.when(below >= 0)
            def _():
                line_copy(i, below, True).wait_recv()

                @pl.when(z < line - 1)
                def _():
                    line_copy(i, below, True).start()

            @pl.when(above < line)
            def _():
                line_copy(i, above, False).wait_recv()

                @pl.when(z > 0)
                def _():
                    line_copy(i, above, False).start()

            return carry

        lax.fori_loop(0, line - 1, step, 0)
        if i + AHEAD < len(chunks):
            line_start(i + AHEAD)

    def act_half(ph, tt, qq, h):
        if ph == 0:
            part = rows // 2
            return acts.at[0, pl.ds(pl.multiple_of(qq * rows + h * part, part), part),
                           pl.ds(pl.multiple_of(tt * cols, cols), cols)]
        part = span // 2
        buf = acts if ph % 2 == 0 else gates
        return buf.at[ph // 2, pl.ds(h * part, part),
                      pl.ds(pl.multiple_of(tt * cols + qq * width, width), width)]

    def own_half(ph, h):
        if ph == 0:
            return tok.at[pl.ds(h * (rows // 2), rows // 2), :]
        return act_half(ph, t, q, h)

    def flip(qq, bits):
        if bits & 1:
            qq = qq + 1 - 2 * (qq % 2)
        if bits & 2:
            qq = qq + 2 - 4 * ((qq // 2) % 2)
        return qq

    directs = ([(1, 0), (1, 1)] if group >= 2 else []) + ([(2, 1), (2, 0)] if group >= 4 else [])
    relays = [(1, 0, 2), (2, 1, 1)] if group >= 4 else []

    def direct_copy(ph, bits, h, sending):
        src = own_half(ph, h)
        dst = act_half(ph, t, q if sending else flip(q, bits), h)
        return remote(src, dst, ag_send.at[ph, bits, h], ag_recv.at[ph, bits, h],
                      (z * group + flip(q, bits), t))

    def relay_copy(ph, origin, h, to, sending):
        part = act_half(ph, t, flip(q, origin if sending else 3), h)
        return remote(part, part, ag_send.at[ph, 3, h], ag_recv.at[ph, 3, h],
                      (z * group + flip(q, to), t))

    def pair_copy(ph, bits, h, d, tt):
        qq = flip(q, bits)
        src = own_half(ph, h) if bits == 0 else act_half(ph, t, qq, h)
        return remote(src, act_half(ph, tt, qq, h), pair_send.at[ph, bits, h, d],
                      pair_recv.at[ph, bits, h, d], in_pair(d))

    def pair_start(ph, bits, h):
        for d in range(1, tps):
            pair_copy(ph, bits, h, d, t).start()

    def gather_start(ph):
        for bits, h in directs:
            direct_copy(ph, bits, h, True).start()
        for h in range(2):
            pair_start(ph, 0, h)

    def gather_relay(ph):
        for origin, h, to in relays:
            direct_copy(ph, origin, h, False).wait_recv()
            relay_copy(ph, origin, h, to, True).start()
        for origin, h, to in relays:
            pair_start(ph, origin, h)

    def gather_finish(ph):
        relayed = [(origin, h) for origin, h, _ in relays]
        for bits, h in directs:
            if (bits, h) not in relayed:
                direct_copy(ph, bits, h, False).wait_recv()
                pair_start(ph, bits, h)
        for origin, h, to in relays:
            relay_copy(ph, origin, h, to, False).wait_recv()
            pair_start(ph, 3, h)
        for bits in range(group):
            for h in range(2):
                for d in range(1, tps):
                    pair_copy(ph, bits, h, d, (t + tps - d) % tps).wait_recv()

    def tiles(body):
        def step(i, carry):
            body(pl.multiple_of(i * tile, tile))
            return carry

        lax.fori_loop(0, span // tile, step, 0)

    def normalize(l):
        sub = 32

        def step(i, carry):
            at = pl.ds(pl.multiple_of(i * sub, sub), sub)
            x = acts[l, at, :].astype(F32)
            scale = lax.rsqrt(jnp.mean(x * x, axis=-1, keepdims=True) + 1e-06)
            normed[at, :] = (x * scale * gain[pl.ds(l, 1), :]).astype(BF16)
            return carry

        lax.fori_loop(0, span // sub, step, 0)

    def project(l, m, r):
        return jnp.dot(normed[pl.ds(r, tile), :], weights[l, m], preferred_element_type=F32).astype(BF16)

    def halo_copy(l):
        return remote(product.at[l, pl.ds(span, 8), :], product.at[l, pl.ds(0, 8), :],
                      halo_send.at[l], halo_recv.at[l], (sp + group, t))

    def do_cgate(l):
        def body(r):
            cgate[pl.ds(r, tile), :] = project(l, 0, r)
        tiles(body)

    def do_values(l):
        def body(r):
            values = project(l, 1, r)
            product[l, pl.ds(r + 8, tile), :] = cgate[pl.ds(r, tile), :].astype(F32) * values.astype(F32)
        tiles(body)

        @pl.when(z < line - 1)
        def _():
            halo_copy(l).start()

    def do_bgate(l):
        @pl.when(z > 0)
        def _():
            halo_copy(l).wait_recv()

        @pl.when(z == 0)
        def _():
            product[l, pl.ds(0, 8), :] = jnp.zeros((8, width), F32)

        tap = [taps[l, pl.ds(k, 1), pl.ds(own, width)] for k in range(3)]

        def body(r):
            bgate = project(l, 2, r).astype(F32)
            near = product[l, pl.ds(r, tile + 8), :]
            mixed = tap[0] * near[6:6 + tile] + tap[1] * near[7:7 + tile] + tap[2] * near[8:8 + tile]
            gates[l, pl.ds(r, tile), pl.ds(own, width)] = (bgate * mixed).astype(BF16)
        tiles(body)

    def out_tile(l):
        def body(r):
            update = jnp.dot(gates[l, pl.ds(r, tile), :], weights[l, 3], preferred_element_type=F32)
            current = (acts[l, pl.ds(r, tile), pl.ds(own, width)].astype(F32) + update).astype(BF16)
            if l + 1 < depth:
                acts[l + 1, pl.ds(r, tile), pl.ds(own, width)] = current
            else:
                result[pl.ds(r, tile), :] = current
        return body

    def do_out(l):
        tiles(out_tile(l))

    def do_out_rows(l, qq):
        body = out_tile(l)
        for k in range(rows // tile):
            body(pl.multiple_of(qq * rows + k * tile, tile))

    def out_copy(d, qq):
        return remote(result.at[pl.ds(pl.multiple_of((q + d) % group * rows, rows), rows), :],
                      landed.at[:, pl.ds(pl.multiple_of(qq * width, width), width)],
                      out_send.at[d], out_recv.at[d], in_plane(d))

    own_tokens = pltpu.make_async_copy(tok, acts.at[0, pl.ds(pl.multiple_of(q * rows, rows), rows), pl.ds(pl.multiple_of(t * cols, cols), cols)], loc_sem.at[len(chunks)])
    own_tokens.start()
    for i in range(len(chunks)):
        if i == min(BEFORE_TOKENS, len(chunks) - 1):
            gather_start(0)
        plane_start(i)
    for i in range(min(AHEAD, len(chunks))):
        line_start(i)
    line_round(0)
    gather_relay(0)
    own_tokens.wait()
    for l in range(depth):
        gather_finish(2 * l)
        normalize(l)
        do_cgate(l)
        if l == 0:
            line_round(1)
        do_values(l)
        line_round(4 * l + 2)
        do_bgate(l)
        gather_start(2 * l + 1)
        gather_relay(2 * l + 1)
        line_round(4 * l + 3)
        if l + 1 < depth:
            line_round(4 * l + 4)
        gather_finish(2 * l + 1)
        if l + 1 < depth:
            do_out(l)
            gather_start(2 * l + 2)
            gather_relay(2 * l + 2)
            line_round(4 * l + 5)
    for d in range(1, group + 1):
        do_out_rows(depth - 1, (q + d) % group)
        if d > 1:
            out_copy(d - 1, q).start()
    landed[:, pl.ds(pl.multiple_of(q * width, width), width)] = result[
        pl.ds(pl.multiple_of(q * rows, rows), rows), :]
    for d in range(1, group):
        out_copy(d, (q + group - d) % group).wait_recv()
    out[...] = landed[...]

    for i in range(len(chunks)):
        for d in range(1, group):
            plane_copy(i, d, q).wait_send()

        def step(zz, carry):
            @pl.when((z < line - 1) & (zz <= z))
            def _():
                line_copy(i, zz, True).wait_send()

            @pl.when((z > 0) & (zz >= z))
            def _():
                line_copy(i, zz, False).wait_send()

            return carry

        lax.fori_loop(0, line, step, 0)
    for ph in range(2 * depth):
        for bits, h in directs:
            direct_copy(ph, bits, h, True).wait_send()
        for origin, h, to in relays:
            relay_copy(ph, origin, h, to, True).wait_send()
        for bits in range(group):
            for h in range(2):
                for d in range(1, tps):
                    pair_copy(ph, bits, h, d, t).wait_send()
    for l in range(depth):
        @pl.when(z < line - 1)
        def _():
            halo_copy(l).wait_send()
    for d in range(1, group):
        out_copy(d, q).wait_send()


def shards(sp_size, tps, tokens, norm_gain, w_bgate, w_cgate, w_value, conv_taps, w_out):
    rows, cols = tokens.shape
    depth, krows, _ = w_bgate.shape
    group = 4
    while group > 1 and (sp_size % group or cols % (group * LANES)):
        group //= 2
    line = sp_size // group
    width = cols // group
    span = rows * group
    full = krows * sp_size
    n = 4 * depth
    dims = (depth, group, line, tps, rows, cols, width, krows)
    anywhere = pl.BlockSpec(memory_space=pl.ANY)
    vmem = pl.BlockSpec(memory_space=pltpu.VMEM)
    dma = pltpu.SemaphoreType.DMA
    return pl.pallas_call(
        functools.partial(mixer_kernel, dims),
        out_shape=jax.ShapeDtypeStruct((rows, cols), BF16),
        in_specs=[anywhere, vmem, anywhere, anywhere, anywhere, vmem, anywhere],
        out_specs=vmem,
        scratch_shapes=[
            pltpu.VMEM((depth, span, full), BF16),
            pltpu.VMEM((depth, span, full), BF16),
            pltpu.VMEM((span, full), BF16),
            pltpu.VMEM((depth, 4, full, width), BF16),
            pltpu.VMEM((depth, span + 8, width), F32),
            pltpu.VMEM((span, width), BF16),
            pltpu.VMEM((span, width), BF16),
            pltpu.VMEM((rows, cols), BF16),
            dma((n + 1,)), dma((n, group)), dma((n, group)),
            dma((2, n, line)), dma((n, line)),
            dma((2 * depth, 4, 2)), dma((2 * depth, 4, 2)),
            dma((2 * depth, group, 2, tps)), dma((2 * depth, group, 2, tps)),
            dma((depth,)), dma((depth,)), dma((group,)), dma((group,)),
        ],
        compiler_params=pltpu.CompilerParams(
            collective_id=0, has_side_effects=True, vmem_limit_bytes=60 * 1024 * 1024),
    )(tokens, norm_gain, w_bgate, w_cgate, w_value, conv_taps, w_out)


def solution(mesh):
    return jax.shard_map(
        functools.partial(shards, mesh.shape["sp"], mesh.shape["tp"]),
        mesh=mesh,
        in_specs=(
            P("sp", "tp"),
            P(),
            P(None, "sp", "tp"),
            P(None, "sp", "tp"),
            P(None, "sp", "tp"),
            P(),
            P(None, "sp", "tp"),
        ),
        out_specs=P("sp", "tp"),
        check_vma=False,
    )
```

```python
import functools

import jax
import jax.numpy as jnp
from jax import lax
from jax.experimental import pallas as pl
from jax.experimental.pallas import tpu as pltpu
from jax.sharding import PartitionSpec as P

MESH = pl.DeviceIdType.MESH
LANES = 128
AHEAD = 2
BEFORE_TOKENS = 2
F32 = jnp.float32
BF16 = jnp.bfloat16


def mixer_kernel(dims, tok, gain, wb, wc, wv, taps, wo, out,
                 acts, gates, normed, weights, product, cgate, result, landed,
                 loc_sem, plane_send, plane_recv, line_send, line_recv,
                 ag_send, ag_recv, pair_send, pair_recv,
                 halo_send, halo_recv, out_send, out_recv):
    depth, group, line, tps, rows, cols, width, krows = dims
    span = rows * group
    block = krows * group
    chunks = [(l, m) for l in range(depth) for m in range(4)]
    sources = (wc, wv, wb, wo)
    sp, t = lax.axis_index("sp"), lax.axis_index("tp")
    z, q = sp // group, sp % group
    own = pl.multiple_of(t * cols + q * width, width)
    tile = min(256, rows)

    def in_plane(d):
        return (z * group + (q + d) % group, t)

    def in_pair(d):
        return (sp, (t + d) % tps)

    def remote(src, dst, send, recv, device):
        return pltpu.make_async_remote_copy(src_ref=src, dst_ref=dst, send_sem=send, recv_sem=recv,
                                            device_id=device, device_id_type=MESH)

    barrier = pltpu.get_barrier_semaphore()

    def hello(device):
        pl.semaphore_signal(barrier, inc=1, device_id=device, device_id_type=MESH)

    for d in range(1, group):
        hello(in_plane(d))
    for d in range(1, tps):
        hello(in_pair(d))

    @pl.when(z > 0)
    def _():
        hello((sp - group, t))

    @pl.when(z < line - 1)
    def _():
        hello((sp + group, t))

    pl.semaphore_wait(barrier, group - 1 + tps - 1
                      + jnp.where(z > 0, 1, 0) + jnp.where(z < line - 1, 1, 0))

    def weight_rows(i, zz, qq):
        l, m = chunks[i]
        return weights.at[l, m, pl.ds(pl.multiple_of((zz * group + qq) * krows, krows), krows), :]

    def weight_block(i, zz):
        l, m = chunks[i]
        return weights.at[l, m, pl.ds(pl.multiple_of(zz * block, block), block), :]

    def weight_source(i, qq):
        l, m = chunks[i]
        return sources[m].at[l, :, pl.ds(pl.multiple_of(qq * width, width), width)]

    def plane_copy(i, d, sender):
        return remote(weight_source(i, (q + d) % group), weight_rows(i, z, sender),
                      plane_send.at[i, d], plane_recv.at[i, d], in_plane(d))

    def local_copy(i):
        return pltpu.make_async_copy(weight_source(i, q), weight_rows(i, z, q), loc_sem.at[i])

    def line_copy(i, zz, up):
        blk = weight_block(i, zz)
        return remote(blk, blk, line_send.at[0 if up else 1, i, zz], line_recv.at[i, zz],
                      (sp + group, t) if up else (sp - group, t))

    def plane_start(i):
        local_copy(i).start()
        for d in range(1, group):
            plane_copy(i, d, q).start()

    def line_start(i):
        local_copy(i).wait()
        for d in range(1, group):
            plane_copy(i, d, (q + group - d) % group).wait_recv()

        @pl.when(z < line - 1)
        def _():
            line_copy(i, z, True).start()

        @pl.when(z > 0)
        def _():
            line_copy(i, z, False).start()

    def line_round(i):
        def step(j, carry):
            below, above = z - 1 - j, z + 1 + j

            @pl.when(below >= 0)
            def _():
                line_copy(i, below, True).wait_recv()

                @pl.when(z < line - 1)
                def _():
                    line_copy(i, below, True).start()

            @pl.when(above < line)
            def _():
                line_copy(i, above, False).wait_recv()

                @pl.when(z > 0)
                def _():
                    line_copy(i, above, False).start()

            return carry

        lax.fori_loop(0, line - 1, step, 0)
        if i + AHEAD < len(chunks) - 1:
            line_start(i + AHEAD)
        if i == len(chunks) - 2:
            line_start(i + 1)

    def act_half(ph, tt, qq, h):
        if ph == 0:
            part = rows // 2
            return acts.at[0, pl.ds(pl.multiple_of(qq * rows + h * part, part), part),
                           pl.ds(pl.multiple_of(tt * cols, cols), cols)]
        part = span // 2
        buf = acts if ph % 2 == 0 else gates
        return buf.at[ph // 2, pl.ds(h * part, part),
                      pl.ds(pl.multiple_of(tt * cols + qq * width, width), width)]

    def own_half(ph, h):
        if ph == 0:
            return tok.at[pl.ds(h * (rows // 2), rows // 2), :]
        return act_half(ph, t, q, h)

    def flip(qq, bits):
        if bits & 1:
            qq = qq + 1 - 2 * (qq % 2)
        if bits & 2:
            qq = qq + 2 - 4 * ((qq // 2) % 2)
        return qq

    directs = ([(1, 0), (1, 1)] if group >= 2 else []) + ([(2, 1), (2, 0)] if group >= 4 else [])
    relays = [(1, 0, 2), (2, 1, 1)] if group >= 4 else []

    def direct_copy(ph, bits, h, sending):
        src = own_half(ph, h)
        dst = act_half(ph, t, q if sending else flip(q, bits), h)
        return remote(src, dst, ag_send.at[ph, bits, h], ag_recv.at[ph, bits, h],
                      (z * group + flip(q, bits), t))

    def relay_copy(ph, origin, h, to, sending):
        part = act_half(ph, t, flip(q, origin if sending else 3), h)
        return remote(part, part, ag_send.at[ph, 3, h], ag_recv.at[ph, 3, h],
                      (z * group + flip(q, to), t))

    def pair_copy(ph, bits, h, d, tt):
        qq = flip(q, bits)
        src = own_half(ph, h) if bits == 0 else act_half(ph, t, qq, h)
        return remote(src, act_half(ph, tt, qq, h), pair_send.at[ph, bits, h, d],
                      pair_recv.at[ph, bits, h, d], in_pair(d))

    def pair_start(ph, bits, h):
        for d in range(1, tps):
            pair_copy(ph, bits, h, d, t).start()

    def gather_start(ph):
        for bits, h in directs:
            direct_copy(ph, bits, h, True).start()
        for h in range(2):
            pair_start(ph, 0, h)

    def gather_relay(ph):
        for origin, h, to in relays:
            direct_copy(ph, origin, h, False).wait_recv()
            relay_copy(ph, origin, h, to, True).start()
        for origin, h, to in relays:
            pair_start(ph, origin, h)

    def gather_finish(ph):
        relayed = [(origin, h) for origin, h, _ in relays]
        for bits, h in directs:
            if (bits, h) not in relayed:
                direct_copy(ph, bits, h, False).wait_recv()
                pair_start(ph, bits, h)
        for origin, h, to in relays:
            relay_copy(ph, origin, h, to, False).wait_recv()
            pair_start(ph, 3, h)
        for bits in range(group):
            for h in range(2):
                for d in range(1, tps):
                    pair_copy(ph, bits, h, d, (t + tps - d) % tps).wait_recv()

    def tiles(body):
        def step(i, carry):
            body(pl.multiple_of(i * tile, tile))
            return carry

        lax.fori_loop(0, span // tile, step, 0)

    def normalize(l):
        sub = 128

        def step(i, carry):
            at = pl.ds(pl.multiple_of(i * sub, sub), sub)
            x = acts[l, at, :].astype(F32)
            scale = lax.rsqrt(jnp.mean(x * x, axis=-1, keepdims=True) + 1e-06)
            normed[at, :] = (x * scale * gain[pl.ds(l, 1), :]).astype(BF16)
            return carry

        lax.fori_loop(0, span // sub, step, 0)

    def project(l, m, r):
        return jnp.dot(normed[pl.ds(r, tile), :], weights[l, m], preferred_element_type=F32).astype(BF16)

    def halo_copy(l):
        return remote(product.at[l, pl.ds(span, 8), :], product.at[l, pl.ds(0, 8), :],
                      halo_send.at[l], halo_recv.at[l], (sp + group, t))

    def do_cgate(l):
        def body(r):
            cgate[pl.ds(r, tile), :] = project(l, 0, r)
        tiles(body)

    def do_values(l):
        def body(r):
            values = project(l, 1, r)
            product[l, pl.ds(r + 8, tile), :] = cgate[pl.ds(r, tile), :].astype(F32) * values.astype(F32)
        tiles(body)

        @pl.when(z < line - 1)
        def _():
            halo_copy(l).start()

    def do_bgate(l):
        @pl.when(z > 0)
        def _():
            halo_copy(l).wait_recv()

        @pl.when(z == 0)
        def _():
            product[l, pl.ds(0, 8), :] = jnp.zeros((8, width), F32)

        tap = [taps[l, pl.ds(k, 1), pl.ds(own, width)] for k in range(3)]

        def body(r):
            bgate = project(l, 2, r).astype(F32)
            near = product[l, pl.ds(r, tile + 8), :]
            mixed = tap[0] * near[6:6 + tile] + tap[1] * near[7:7 + tile] + tap[2] * near[8:8 + tile]
            gates[l, pl.ds(r, tile), pl.ds(own, width)] = (bgate * mixed).astype(BF16)
        tiles(body)

    def out_tile(l):
        def body(r):
            update = jnp.dot(gates[l, pl.ds(r, tile), :], weights[l, 3], preferred_element_type=F32)
            current = (acts[l, pl.ds(r, tile), pl.ds(own, width)].astype(F32) + update).astype(BF16)
            if l + 1 < depth:
                acts[l + 1, pl.ds(r, tile), pl.ds(own, width)] = current
            else:
                result[pl.ds(r, tile), :] = current
        return body

    def do_out(l):
        tiles(out_tile(l))

    def do_out_rows(l, qq):
        body = out_tile(l)
        for k in range(rows // tile):
            body(pl.multiple_of(qq * rows + k * tile, tile))

    def out_copy(d, qq):
        return remote(result.at[pl.ds(pl.multiple_of((q + d) % group * rows, rows), rows), :],
                      landed.at[:, pl.ds(pl.multiple_of(qq * width, width), width)],
                      out_send.at[d], out_recv.at[d], in_plane(d))

    own_tokens = pltpu.make_async_copy(tok, acts.at[0, pl.ds(pl.multiple_of(q * rows, rows), rows), pl.ds(pl.multiple_of(t * cols, cols), cols)], loc_sem.at[len(chunks)])
    own_tokens.start()
    for i in range(len(chunks)):
        if i == min(BEFORE_TOKENS, len(chunks) - 1):
            gather_start(0)
        plane_start(i)
    for i in range(min(AHEAD, len(chunks))):
        line_start(i)
    line_round(0)
    gather_relay(0)
    own_tokens.wait()
    for l in range(depth):
        gather_finish(2 * l)
        normalize(l)
        do_cgate(l)
        if l == 0:
            line_round(1)
        do_values(l)
        line_round(4 * l + 2)
        do_bgate(l)
        gather_start(2 * l + 1)
        gather_relay(2 * l + 1)
        line_round(4 * l + 3)
        gather_finish(2 * l + 1)
        if l + 1 < depth:
            do_out(l)
            line_round(4 * l + 4)
            gather_start(2 * l + 2)
            gather_relay(2 * l + 2)
            line_round(4 * l + 5)
    for d in range(1, group + 1):
        do_out_rows(depth - 1, (q + d) % group)
        if d > 1:
            out_copy(d - 1, q).start()
    landed[:, pl.ds(pl.multiple_of(q * width, width), width)] = result[
        pl.ds(pl.multiple_of(q * rows, rows), rows), :]
    for d in range(1, group):
        out_copy(d, (q + group - d) % group).wait_recv()
    out[...] = landed[...]

    for i in range(len(chunks)):
        for d in range(1, group):
            plane_copy(i, d, q).wait_send()

        def step(zz, carry):
            @pl.when((z < line - 1) & (zz <= z))
            def _():
                line_copy(i, zz, True).wait_send()

            @pl.when((z > 0) & (zz >= z))
            def _():
                line_copy(i, zz, False).wait_send()

            return carry

        lax.fori_loop(0, line, step, 0)
    for ph in range(2 * depth):
        for bits, h in directs:
            direct_copy(ph, bits, h, True).wait_send()
        for origin, h, to in relays:
            relay_copy(ph, origin, h, to, True).wait_send()
        for bits in range(group):
            for h in range(2):
                for d in range(1, tps):
                    pair_copy(ph, bits, h, d, t).wait_send()
    for l in range(depth):
        @pl.when(z < line - 1)
        def _():
            halo_copy(l).wait_send()
    for d in range(1, group):
        out_copy(d, q).wait_send()


def shards(sp_size, tps, tokens, norm_gain, w_bgate, w_cgate, w_value, conv_taps, w_out):
    rows, cols = tokens.shape
    depth, krows, _ = w_bgate.shape
    group = 4
    while group > 1 and (sp_size % group or cols % (group * LANES)):
        group //= 2
    line = sp_size // group
    width = cols // group
    span = rows * group
    full = krows * sp_size
    n = 4 * depth
    dims = (depth, group, line, tps, rows, cols, width, krows)
    anywhere = pl.BlockSpec(memory_space=pl.ANY)
    vmem = pl.BlockSpec(memory_space=pltpu.VMEM)
    dma = pltpu.SemaphoreType.DMA
    return pl.pallas_call(
        functools.partial(mixer_kernel, dims),
        out_shape=jax.ShapeDtypeStruct((rows, cols), BF16),
        in_specs=[anywhere, vmem, anywhere, anywhere, anywhere, vmem, anywhere],
        out_specs=vmem,
        scratch_shapes=[
            pltpu.VMEM((depth, span, full), BF16),
            pltpu.VMEM((depth, span, full), BF16),
            pltpu.VMEM((span, full), BF16),
            pltpu.VMEM((depth, 4, full, width), BF16),
            pltpu.VMEM((depth, span + 8, width), F32),
            pltpu.VMEM((span, width), BF16),
            pltpu.VMEM((span, width), BF16),
            pltpu.VMEM((rows, cols), BF16),
            dma((n + 1,)), dma((n, group)), dma((n, group)),
            dma((2, n, line)), dma((n, line)),
            dma((2 * depth, 4, 2)), dma((2 * depth, 4, 2)),
            dma((2 * depth, group, 2, tps)), dma((2 * depth, group, 2, tps)),
            dma((depth,)), dma((depth,)), dma((group,)), dma((group,)),
        ],
        compiler_params=pltpu.CompilerParams(
            collective_id=0, has_side_effects=True, vmem_limit_bytes=60 * 1024 * 1024),
    )(tokens, norm_gain, w_bgate, w_cgate, w_value, conv_taps, w_out)


def solution(mesh):
    return jax.shard_map(
        functools.partial(shards, mesh.shape["sp"], mesh.shape["tp"]),
        mesh=mesh,
        in_specs=(
            P("sp", "tp"),
            P(),
            P(None, "sp", "tp"),
            P(None, "sp", "tp"),
            P(None, "sp", "tp"),
            P(),
            P(None, "sp", "tp"),
        ),
        out_specs=P("sp", "tp"),
        check_vma=False,
    )
```
